32 devices in a mesh: sp: 8 (over z, x), tp: 4 (over y, core).
Axes of the slice: x: 2, y: 2, z: 4, core: 2. Of those that a mesh axis runs over, the one named last changes fastest.
Arguments:
- signal: bfloat16 [1024, 1024], P('sp', 'tp'), may hold values from -6 to 6
- step_log: float32 [1024, 64], P('sp', 'tp'), may hold values from -9 to -1.9
- forget_log: float32 [1024, 64], P('sp', 'tp'), may hold values from -1.4 to 0
- damping: float32 [64, 64], P('tp'), may hold values from 0.001 to 1.6
- freq: float32 [64, 64], P('tp'), may hold values from 0 to 50.26544
- in_re: bfloat16 [64, 64, 16], P('tp'), may hold values from -1 to 1
- in_im: bfloat16 [64, 64, 16], P('tp'), may hold values from -1 to 1
- out_re: bfloat16 [64, 16, 64], P('tp'), may hold values from -4 to 4
- out_im: bfloat16 [64, 16, 64], P('tp'), may hold values from -4 to 4
- skip: float32 [1024], P('tp'), may hold values from -4 to 4
- w_out: bfloat16 [1024, 2048], P('tp'), may hold values from -0.1875 to 0.1875
- residual: bfloat16 [1024, 2048], P('sp', 'tp'), may hold values from -60 to 60
- norm_gain: bfloat16 [2048], P('tp'), may hold values from 0.099609375 to 1.8984375
- w_gate: bfloat16 [2048, 5632], P('sp', 'tp'), may hold values from -0.125 to 0.125
- w_up: bfloat16 [2048, 5632], P('sp', 'tp'), may hold values from -0.125 to 0.125
- w_down: bfloat16 [5632, 2048], P('tp', 'sp'), may hold values from -0.078125 to 0.078125
Outputs:
- output: bfloat16 [1024, 2048], P('sp', 'tp')
The draws below stay inside these ranges and needn't reach their ends.
All inputs are finite; a program needn't handle non-finite values.
Results may differ from the reference program's by a relative error of at most 0.012.
Values may be sent and summed in bfloat16 or wider, within the bound.
A program may use at most 64 MiB of HBM per device.

```python
import math
import jax
import jax.numpy as jnp
from jax import lax

D = 2048
SSM_W = 1024
FF = 5632
SSM_GROUP = 16
STATE = 64
TOK_DEV = 128
GROUPS = 64
TOKENS = 1024
N_SP = 8
N_TP = 4


def slow_groups(key):
    share = 0.5
    return jax.random.bernoulli(jax.random.fold_in(key, 101), share, (GROUPS,))


def draw_step_log(key, part):
    slow = slow_groups(key)
    base = jnp.where(slow, 0.5 * jnp.log(0.035 / TOKENS), jnp.log(0.05)).astype(jnp.float32)
    blocks = jax.random.uniform(jax.random.fold_in(key, 102), (TOKENS // TOK_DEV, GROUPS), jnp.float32, -0.7, 0.7)
    spread = jnp.repeat(blocks, TOK_DEV, axis=0)
    rough = jax.random.uniform(jax.random.fold_in(key, 103), (TOKENS, GROUPS), jnp.float32, -0.35, 0.35)
    return (base[None, :] + spread + rough).astype(jnp.float32)


def draw_damping(key, part):
    slow = slow_groups(key)
    fast_rate = jnp.exp(jax.random.uniform(jax.random.fold_in(key, 104), (GROUPS, STATE), jnp.float32, math.log(0.6), math.log(1.6)))
    slow_rate = jnp.exp(jax.random.uniform(jax.random.fold_in(key, 105), (GROUPS, STATE), jnp.float32, math.log(0.2), math.log(0.8))) / jnp.sqrt(0.035 * TOKENS)
    return jnp.where(slow[:, None], slow_rate, fast_rate).astype(jnp.float32)


def draw_forget_log(key, part):
    places = jax.random.randint(jax.random.fold_in(key, 106), (3, GROUPS), 0, TOKENS)
    depth = jax.random.uniform(jax.random.fold_in(key, 107), (3, GROUPS), jnp.float32, math.log(0.65), math.log(0.8))
    positions = jnp.arange(TOKENS)[:, None, None]
    hits = positions == places[None, :, :]
    return jnp.sum(jnp.where(hits, depth[None, :, :], 0.0), axis=1).astype(jnp.float32)


def draw_residual(key, part):
    base = jnp.clip(jax.random.normal(jax.random.fold_in(key, 108), (TOKENS, D), jnp.float32), -6.0, 6.0)
    rough = jax.random.uniform(jax.random.fold_in(key, 109), (D,), jnp.float32, -0.35, 0.35)
    columns = jnp.exp(math.log(4.0) * jnp.arange(D, dtype=jnp.float32) / D + rough)
    scales = jnp.exp(jax.random.uniform(jax.random.fold_in(key, 110), (TOKENS, 1), jnp.float32, -0.35, 0.35))
    return (0.5 * base * scales * columns[None, :]).astype(jnp.bfloat16)


def levels(key, dims, pieces, least, top_value):
    level = 1.0
    for axis_at, shards_of in pieces:
        steps = jax.random.uniform(jax.random.fold_in(jax.random.fold_in(key, 6), axis_at), (shards_of,), jnp.float32, least / len(pieces), top_value / len(pieces))
        level = level * jnp.repeat(jnp.exp(steps), dims[axis_at] // shards_of).reshape((-1,) + (1,) * (len(dims) - 1 - axis_at))
    return level


def gaussian(own_key, extent, scale, reach, split=(), held_as=jnp.bfloat16):
    entries = scale * jax.random.normal(own_key, extent, jnp.float32)
    if split:
        entries = entries * levels(own_key, extent, split, -0.22, 0.18)
    return jnp.clip(entries, -reach, reach).astype(held_as)


def setup_inputs(seed: int = 0) -> dict:
    key_list = jax.random.split(jax.random.key(seed), 17)
    signal = gaussian(key_list[0], (TOKENS, SSM_W), 1.0, 6.0, ((0, 8), (1, 4)))
    step_log = draw_step_log(jax.random.fold_in(key_list[16], 71), 0)
    forget_log = draw_forget_log(jax.random.fold_in(key_list[16], 71), 0)
    damping = draw_damping(jax.random.fold_in(key_list[16], 71), 0)
    freq = jnp.clip(50.26544 * jax.random.uniform(key_list[4], (GROUPS, STATE), jnp.float32) ** levels(key_list[4], (GROUPS, STATE), ((0, 4),), -0.2, 0.2), 0.0, 50.26544)
    in_re = gaussian(key_list[5], (GROUPS, STATE, SSM_GROUP), (2 * SSM_GROUP) ** -0.5, 1.0, ((0, 4),))
    in_im = gaussian(key_list[6], (GROUPS, STATE, SSM_GROUP), (2 * SSM_GROUP) ** -0.5, 1.0, ((0, 4),))
    out_re = gaussian(key_list[7], (GROUPS, SSM_GROUP, STATE), 1.0, 4.0, ((0, 4),))
    out_im = gaussian(key_list[8], (GROUPS, SSM_GROUP, STATE), 1.0, 4.0, ((0, 4),))
    skip = gaussian(key_list[9], (SSM_W,), 1.0, 4.0, ((0, 4),), jnp.float32)
    w_out = gaussian(key_list[10], (SSM_W, D), SSM_W ** -0.5, 0.1875, ((0, 4),))
    residual = draw_residual(jax.random.fold_in(key_list[16], 71), 0)
    norm_gain = jnp.clip(1.0 + 0.18 * jax.random.normal(key_list[12], (D,), jnp.float32), 0.099609375, 1.8984375).astype(jnp.bfloat16)
    w_gate = gaussian(key_list[13], (D, FF), D ** -0.5, 0.125, ((0, 8), (1, 4)))
    w_up = gaussian(key_list[14], (D, FF), D ** -0.5, 0.125, ((0, 8), (1, 4)))
    w_down = gaussian(key_list[15], (FF, D), FF ** -0.5, 0.078125, ((0, 4), (1, 8)))
    return dict(signal=signal, step_log=step_log, forget_log=forget_log, damping=damping, freq=freq, in_re=in_re, in_im=in_im, out_re=out_re, out_im=out_im, skip=skip, w_out=w_out, residual=residual, norm_gain=norm_gain, w_gate=w_gate, w_up=w_up, w_down=w_down)


EPS = 1e-06

def state_mixer(signal, step_log, forget_log, damping, freq, in_re, in_im, out_re, out_im, skip):
    length = signal.shape[0]
    groups, states = damping.shape
    width = in_re.shape[2]
    rows = signal.astype(jnp.float32).reshape(length, groups, width)
    weight_re = in_re.astype(jnp.float32)
    weight_im = in_im.astype(jnp.float32)
    readout_real = out_re.astype(jnp.float32)
    readout_imaginary = out_im.astype(jnp.float32)
    denom = damping * damping + freq * freq

    def advance(carry, inputs):
        state_re, state_im = carry
        row, log_step, forget = inputs
        step = jnp.exp(log_step)[:, None]
        magnitude = jnp.exp(-damping * step)
        angle = freq * step
        decay_re = magnitude * jnp.cos(angle)
        decay_im = magnitude * jnp.sin(angle)
        factor_re = (-(decay_re - 1.0) * damping + decay_im * freq) / denom
        factor_im = (-decay_im * damping - (decay_re - 1.0) * freq) / denom
        keep = jnp.exp(forget)[:, None]
        source_re = jnp.einsum('gpc,gc->gp', weight_re, row, precision=lax.Precision.HIGHEST)
        source_im = jnp.einsum('gpc,gc->gp', weight_im, row, precision=lax.Precision.HIGHEST)
        drive_re = factor_re * source_re - factor_im * source_im
        drive_im = factor_re * source_im + factor_im * source_re
        following_real = keep * (decay_re * state_re - decay_im * state_im) + drive_re
        following_imaginary = keep * (decay_re * state_im + decay_im * state_re) + drive_im
        state_readout = jnp.einsum('kuy,ky->ku', readout_real, following_real, precision=lax.Precision.HIGHEST) - jnp.einsum('kuy,ky->ku', readout_imaginary, following_imaginary, precision=lax.Precision.HIGHEST)
        return ((following_real, following_imaginary), state_readout.reshape(groups * width))
    anchor = jnp.zeros((groups, states), jnp.float32)
    _, readouts = lax.scan(advance, (anchor, anchor), (rows, step_log, forget_log))
    value = readouts + skip * signal.astype(jnp.float32)
    return jax.nn.gelu(value).astype(jnp.bfloat16)

def block_sum(left, right, parts):
    span = left.shape[1] // parts
    total = jnp.zeros((left.shape[0], right.shape[1]), jnp.float32)
    for number in range(parts):
        term = jnp.dot(left[:, number * span:(number + 1) * span], right[number * span:(number + 1) * span], preferred_element_type=jnp.float32)
        rounded = lax.optimization_barrier(term.astype(jnp.bfloat16))
        total = total + rounded.astype(jnp.float32)
    return total

def reference(signal, step_log, forget_log, damping, freq, in_re, in_im, out_re, out_im, skip, w_out, residual, norm_gain, w_gate, w_up, w_down):
    mixed = state_mixer(signal, step_log, forget_log, damping, freq, in_re, in_im, out_re, out_im, skip)

    def finish(items):
        mixed_rows, resid_rows = items
        projected = block_sum(mixed_rows, w_out, N_TP)
        middle = (resid_rows.astype(jnp.float32) + projected).astype(jnp.bfloat16)
        middle_wide = middle.astype(jnp.float32)
        mean_square = lax.optimization_barrier(jnp.mean(middle_wide * middle_wide, axis=1, keepdims=True))
        normed = (middle_wide * lax.rsqrt(mean_square + EPS) * norm_gain.astype(jnp.float32)).astype(jnp.bfloat16)
        gate = jnp.dot(normed, w_gate, preferred_element_type=jnp.float32)
        up_projected = jnp.dot(normed, w_up, preferred_element_type=jnp.float32)
        hidden = (jax.nn.silu(gate) * up_projected).astype(jnp.bfloat16)
        down = block_sum(hidden, w_down, N_TP)
        return (middle_wide + 0.5 * down).astype(jnp.bfloat16)
    outputs = lax.map(finish, (mixed.reshape(N_SP, TOK_DEV, mixed.shape[1]), residual.reshape(N_SP, TOK_DEV, residual.shape[1])))
    return outputs.reshape(residual.shape)
```

```python
import functools

import jax
import jax.numpy as jnp
from jax import lax
from jax.experimental import pallas as pl
from jax.experimental.pallas import tpu as pltpu
from jax.sharding import PartitionSpec as P

EPS = 1e-06


def entering(value, axis, join, neutral):
    count, mine = (lax.axis_size(axis), lax.axis_index(axis))
    pieces = jax.tree.map(lambda part: lax.all_gather(part, axis), value)
    subtotal = jax.tree.map(
        lambda part, zero: jnp.full_like(part, 0) + jnp.asarray(zero, part.dtype), value, neutral
    )

    def turn(position, subtotal):
        longer = join(subtotal, jax.tree.map(lambda part: part[position], pieces))
        return jax.tree.map(lambda new, old: jnp.where(position < mine, new, old), longer, subtotal)

    return lax.fori_loop(0, count - 1, turn, subtotal)


def combine(earlier, later):
    first_are, first_aim, first_bre, first_bim = earlier
    second_are, second_aim, second_bre, second_bim = later
    return (
        second_are * first_are - second_aim * first_aim,
        second_are * first_aim + second_aim * first_are,
        second_are * first_bre - second_aim * first_bim + second_bre,
        second_are * first_bim + second_aim * first_bre + second_bim,
    )


def collect(w_gate, w_up, w_down):
    gate_values_wide, up_full = (
        lax.all_gather(w_gate, "sp", axis=0, tiled=True),
        lax.all_gather(w_up, "sp", axis=0, tiled=True),
    )
    down_full = lax.all_gather(w_down, "sp", axis=1, tiled=True)
    return (gate_values_wide, up_full, down_full)


def local_states(elements, length, flat):
    span = 8
    blocks = tuple((item.reshape(length // span, span, flat) for item in elements))

    def advance(carry, block):
        collected = []
        for offset in range(span):
            carry = combine(carry, tuple((member[offset] for member in block)))
            collected.append(carry)
        stacked = tuple((jnp.stack([entry[number] for entry in collected]) for number in range(4)))
        return (carry, stacked)

    unity = jnp.ones((flat,), jnp.float32)
    nothing = jnp.zeros((flat,), jnp.float32)
    finals, stacked = lax.scan(advance, (unity, nothing, nothing, nothing), blocks)
    return (finals, tuple((member.reshape(length, flat) for member in stacked)))


def state_mixer(signal, step_log, forget_log, damping, freq, in_re, in_im, out_re, out_im, skip):
    length = signal.shape[0]
    groups, states = damping.shape
    width = in_re.shape[2]
    step = jnp.exp(step_log)[:, :, None]
    magnitude = jnp.exp(-damping[None] * step)
    angle = freq[None] * step
    decay_re = magnitude * jnp.cos(angle)
    decay_im = magnitude * jnp.sin(angle)
    denom = damping * damping + freq * freq
    factor_re = (-(decay_re - 1.0) * damping + decay_im * freq) / denom
    factor_im = (-decay_im * damping - (decay_re - 1.0) * freq) / denom
    keep = jnp.exp(forget_log)[:, :, None]
    rows = signal.reshape(length, groups, width)
    both_in = jnp.concatenate([in_re, in_im], axis=1)
    driven = jnp.einsum("tgc,gpc->tgp", rows, both_in, preferred_element_type=jnp.float32)
    source_re = driven[:, :, :states]
    source_im = driven[:, :, states:]
    drive_re = factor_re * source_re - factor_im * source_im
    drive_im = factor_re * source_im + factor_im * source_re
    flat = groups * states
    elements = (
        (keep * decay_re).reshape(length, flat),
        (keep * decay_im).reshape(length, flat),
        drive_re.reshape(length, flat),
        drive_im.reshape(length, flat),
    )
    finals, (running_real, cum_im, local_re, local_im) = local_states(elements, length, flat)
    unity = jnp.ones((flat,), jnp.float32)
    nothing = jnp.zeros((flat,), jnp.float32)
    prior = entering(finals, "sp", combine, (unity, nothing, nothing, nothing))
    state_re = local_re + running_real * prior[2][None] - cum_im * prior[3][None]
    state_im = local_im + running_real * prior[3][None] + cum_im * prior[2][None]
    state_readout = jnp.einsum(
        "myq,yzq->myz",
        state_re.reshape(length, groups, states),
        out_re.astype(jnp.float32),
        precision=lax.Precision.HIGHEST,
    ) - jnp.einsum(
        "myq,yzq->myz",
        state_im.reshape(length, groups, states),
        out_im.astype(jnp.float32),
        precision=lax.Precision.HIGHEST,
    )
    value = state_readout.reshape(length, groups * width) + skip * signal.astype(jnp.float32)
    return jax.nn.gelu(value).astype(jnp.bfloat16)


def local(
    signal,
    step_log,
    forget_log,
    damping,
    freq,
    in_re,
    in_im,
    out_re,
    out_im,
    skip,
    w_out,
    residual,
    norm_gain,
    w_gate,
    w_up,
    w_down,
):
    mixed = state_mixer(
        signal, step_log, forget_log, damping, freq, in_re, in_im, out_re, out_im, skip
    )
    partial_value = jnp.dot(mixed, w_out, preferred_element_type=jnp.float32)
    gate_values_wide, up_full, down_full = collect(w_gate, w_up, w_down)
    model_width = w_out.shape[1]
    projected = lax.psum_scatter(
        partial_value.astype(jnp.bfloat16), "tp", scatter_dimension=1, tiled=True
    ).astype(jnp.float32)
    middle = (residual.astype(jnp.float32) + projected).astype(jnp.bfloat16)
    middle_wide = middle.astype(jnp.float32)
    squares = lax.psum(jnp.sum(middle_wide * middle_wide, axis=1), "tp")
    normed = (
        middle_wide
        * lax.rsqrt(squares[:, None] / model_width + EPS)
        * norm_gain.astype(jnp.float32)
    ).astype(jnp.bfloat16)
    piece = lax.all_gather(normed, "tp", axis=1, tiled=True)
    gate = jnp.dot(piece, gate_values_wide, preferred_element_type=jnp.float32)
    up_projected = jnp.dot(piece, up_full, preferred_element_type=jnp.float32)
    hidden = (jax.nn.silu(gate) * up_projected).astype(jnp.bfloat16)
    down_terms = jnp.dot(hidden, down_full, preferred_element_type=jnp.float32)
    down = lax.psum_scatter(
        down_terms.astype(jnp.bfloat16), "tp", scatter_dimension=1, tiled=True
    ).astype(jnp.float32)
    return (middle_wide + 0.5 * down).astype(jnp.bfloat16)

MESH = pl.DeviceIdType.MESH
F32 = jnp.float32
BF16 = jnp.bfloat16
NT = (((1,), (1,)), ((), ()))


def sincos(angle):
    turns = jnp.floor(angle * 0.6366197723675814 + 0.5)
    r = angle - turns * 1.5703125
    r = r - turns * 4.837512969970703125e-4
    r = r - turns * 7.54978995489188216e-8
    q = turns.astype(jnp.int32)
    r2 = r * r
    s = ((-1.9515295891e-4 * r2 + 8.3321608736e-3) * r2 - 1.6666654611e-1) * r2 * r + r
    c = (
        ((2.443315711809948e-5 * r2 - 1.388731625493765e-3) * r2 + 4.166664568298827e-2) * r2 * r2
        - 0.5 * r2
        + 1.0
    )
    swap = (q & 1) == 1
    sine = jnp.where(swap, c, s)
    cosine = jnp.where(swap, s, c)
    sine = jnp.where((q & 2) == 2, -sine, sine)
    cosine = jnp.where(((q + 1) & 2) == 2, -cosine, cosine)
    return sine, cosine


def log2(n):
    return n.bit_length() - 1


def fused_kernel(
    S, T, X, C,
    signal, step_log, forget_log, damping, freq, b_re, b_im, c_re, c_im, skip, w_out, residual, gain,
    wg, wu, wd, out,
    stepx, keepx, dre, dim, lre, lim, rre, rim, fin, finr, part, partr, ssq, ssqr,
    wgr, wur, wdr, nbuf, mid, pbuf, rc, ry, rx, rz, send_sems, recv_sems,
):
    Z, Y = S // X, T // C
    s, t = lax.axis_index("sp"), lax.axis_index("tp")
    z, x = lax.div(s, X), lax.rem(s, X)
    y, c = lax.div(t, C), lax.rem(t, C)
    rows, chans = signal.shape
    flat = damping.shape[1]
    groups = step_log.shape[1]
    states, width = flat // groups, chans // groups
    piece, ks = wgr.shape[1:]
    kt = nbuf.shape[2]
    model = T * kt
    count = [0]
    copies = []

    def send(src, dst, **where):
        k = count[0]
        count[0] += 1
        copy = pltpu.make_async_remote_copy(
            src_ref=src, dst_ref=dst, send_sem=send_sems.at[k], recv_sem=recv_sems.at[k],
            device_id=where, device_id_type=MESH,
        )
        copy.start()
        copies.append(copy)
        return copy

    barrier = pltpu.get_barrier_semaphore()
    for d in range(1, S):
        pl.semaphore_signal(barrier, inc=1, device_id={"sp": lax.rem(s + d, S)}, device_id_type=MESH)
    for d in range(1, T):
        pl.semaphore_signal(barrier, inc=1, device_id={"tp": lax.rem(t + d, T)}, device_id_type=MESH)
    pl.semaphore_wait(barrier, S + T - 2)

    def spread(weight, landing):
        sent = []
        for d in range(1, S):
            to = lax.rem(s + d, S)
            sent.append(send(weight.at[pl.ds(to * piece, piece)], landing.at[s], sp=to))
        landing[s] = weight[pl.ds(pl.multiple_of(s * piece, 16), piece)]
        return sent

    gate_copies = spread(wg, wgr)

    lane = lax.broadcasted_iota(jnp.int32, (groups, flat), 1)
    grow = lax.broadcasted_iota(jnp.int32, (groups, flat), 0)
    onehot = jnp.where((lane >> log2(states)) == grow, 1.0, 0.0).astype(F32)
    stepx[...] = jnp.dot(jnp.exp(step_log[...]), onehot, precision=lax.Precision.HIGHEST,
                         preferred_element_type=F32)
    keepx[...] = jnp.dot(jnp.exp(forget_log[...]), onehot, precision=lax.Precision.HIGHEST,
                         preferred_element_type=F32)
    wide = lax.broadcasted_iota(jnp.int32, (chans, flat), 1) >> log2(states)
    tall = lax.broadcasted_iota(jnp.int32, (chans, flat), 0) >> log2(width)
    own = wide == tall

    def block_diagonal(ref):
        value = ref[...].astype(F32)
        value = jnp.concatenate([value] * (flat // value.shape[1]), axis=1)
        return jnp.where(own, value, 0.0).astype(BF16)

    dre[...] = jnp.dot(signal[...], block_diagonal(b_re), preferred_element_type=F32)
    dim[...] = jnp.dot(signal[...], block_diagonal(b_im), preferred_element_type=F32)
    denom = damping[...] * damping[...] + freq[...] * freq[...]
    dn, fn = damping[...] / denom, freq[...] / denom
    sub = lax.broadcasted_iota(jnp.int32, (8, flat), 0)

    def block(i, carry):
        at = pl.ds(pl.multiple_of(i * 8, 8), 8)
        st, kp = stepx[at, :], keepx[at, :]
        mag = jnp.exp(-damping[...] * st)
        sine, cosine = sincos(freq[...] * st)
        zr, zi = mag * cosine, mag * sine
        fr = zi * fn - (zr - 1.0) * dn
        fi = -zi * dn - (zr - 1.0) * fn
        sr, si = dre[at, :], dim[at, :]
        value = (kp * zr, kp * zi, fr * sr - fi * si, fr * si + fi * sr)
        for d in (1, 2, 4):
            ok = sub >= d
            before = tuple(
                jnp.where(ok, pltpu.roll(v, d, 0), n) for v, n in zip(value, (1.0, 0.0, 0.0, 0.0))
            )
            value = combine(before, value)
        value = combine(carry, value)
        rre[at, :], rim[at, :], lre[at, :], lim[at, :] = value
        return tuple(v[7:8, :] for v in value)

    one, nil = jnp.ones((1, flat), F32), jnp.zeros((1, flat), F32)
    final = lax.fori_loop(0, rows // 8, block, (one, nil, nil, nil))
    fold = flat // 128
    for a in range(4):
        for k in range(fold):
            fin[a, k:k + 1, :] = final[a][:, k * 128:(k + 1) * 128]
    final_copies = []
    for d in range(1, S):
        final_copies.append(send(fin, finr.at[s], sp=lax.rem(s + d, S)))
    up_copies = spread(wu, wur)
    for copy in final_copies:
        copy.wait_recv()
    prior = (jnp.ones((fold, 128), F32),) + (jnp.zeros((fold, 128), F32),) * 3
    for p in range(S - 1):
        longer = combine(prior, tuple(finr[p, a] for a in range(4)))
        prior = tuple(jnp.where(p < s, n, o) for n, o in zip(longer, prior))
    pre, pim = (
        jnp.concatenate([v[k:k + 1, :] for k in range(fold)], axis=1) for v in prior[2:]
    )

    @pl.loop(0, rows // 32)
    def _(i):
        at = pl.ds(pl.multiple_of(i * 32, 32), 32)
        ar, ai = rre[at, :], rim[at, :]
        lre[at, :] = lre[at, :] + ar * pre - ai * pim
        lim[at, :] = lim[at, :] + ar * pim + ai * pre

    def readout(state, matrix):
        high = state.astype(BF16)
        low = (state - high.astype(F32)).astype(BF16)
        return lax.dot_general(high, matrix, NT, preferred_element_type=F32) + lax.dot_general(
            low, matrix, NT, preferred_element_type=F32
        )

    value = readout(lre[...], block_diagonal(c_re)) - readout(lim[...], block_diagonal(c_im))
    value = value + skip[...] * signal[...].astype(F32)
    mixed = jax.nn.gelu(value).astype(BF16)

    part_copies = []
    for b in range(T):
        part[b] = jnp.dot(
            mixed, w_out[:, b * kt:(b + 1) * kt], preferred_element_type=F32
        ).astype(BF16)
    for d in range(1, T):
        to = lax.rem(t + d, T)
        part_copies.append(send(part.at[to], partr.at[d], tp=to))
    total = part[t].astype(F32)
    for d in range(1, T):
        part_copies[d - 1].wait_recv()
        total = total + partr[d].astype(F32)
    middle = (residual[...].astype(F32) + total).astype(BF16)
    mid[...] = middle
    wide_mid = middle.astype(F32)
    ssq[...] = lax.dot_general(
        jnp.ones((8, kt), F32), wide_mid * wide_mid, NT,
        precision=lax.Precision.HIGHEST, preferred_element_type=F32,
    )
    ssq_copies = [send(ssq, ssqr.at[d], tp=lax.rem(t + d, T)) for d in range(1, T)]
    squares = ssq[...]
    for d in range(1, T):
        ssq_copies[d - 1].wait_recv()
        squares = squares + ssqr[d]
    eye = lax.broadcasted_iota(jnp.int32, (rows, rows), 0) == lax.broadcasted_iota(
        jnp.int32, (rows, rows), 1
    )
    squares = jnp.sum(jnp.where(eye, squares[0:1, :], 0.0), axis=1, keepdims=True)
    normed = mid[...].astype(F32) * lax.rsqrt(squares / model + EPS) * gain[...].astype(F32)
    here = pl.ds(pl.multiple_of(s * rows, rows), rows)
    nbuf[t, here, :] = normed.astype(BF16)

    def tokens(zz, xx):
        return pl.ds(pl.multiple_of((zz * X + xx) * rows, rows), rows)

    def pass_on(block_ref, **where):
        return send(block_ref, block_ref, **where)

    mine = nbuf.at[t, here]
    z_copies = [None] + [
        pass_on(mine, sp=lax.rem(z + d, Z) * X + x) for d in range(1, Z)
    ]
    down_copies = spread(wd, wdr)
    across = [(e, z * X + lax.rem(x + e, X)) for e in range(1, X)]
    ups = [(e, lax.rem(y + e, Y) * C + c) for e in range(1, Y)]
    mates = [(e, y * C + lax.rem(c + e, C)) for e in range(1, C)]
    y_copies, c_copies = [], []

    def to_tp(zz, xx):
        block_ref = nbuf.at[t, tokens(zz, xx)]
        for e, to in ups:
            back = lax.rem(y - e + Y, Y) * C + c
            y_copies.append((pass_on(block_ref, tp=to), nbuf.at[back, tokens(zz, xx)]))
        for e, to in mates:
            c_copies.append(pass_on(block_ref, tp=to))

    done = [0]

    def flush_y(upto):
        while done[0] < upto:
            copy, block_ref = y_copies[done[0]]
            copy.wait_recv()
            for e, to in mates:
                c_copies.append(pass_on(block_ref, tp=to))
            done[0] += 1

    for d in range(Z):
        zz = lax.rem(z - d + Z, Z)
        if d:
            z_copies[d].wait_recv()
        x_copies = [
            pass_on(nbuf.at[t, tokens(zz, x)], sp=z * X + lax.rem(x + e, X)) for e in range(1, X)
        ]
        to_tp(zz, x)
        for e in range(1, X):
            x_copies[e - 1].wait_recv()
            to_tp(zz, lax.rem(x - e + X, X))
        flush_y(len(y_copies) - X * (Y - 1))
    flush_y(len(y_copies))
    for copy in gate_copies + up_copies + c_copies:
        copy.wait_recv()

    span = X * rows
    order = [d for d in range(1, Z)] + [0]
    first, second, third, fourth = {}, {}, {}, {}

    def at_z(d):
        return pl.ds(pl.multiple_of(lax.rem(z + d, Z) * span, span), span)

    def stage_hidden(d):
        at = at_z(d)
        gate = jnp.zeros((span, piece), F32)
        up = jnp.zeros((span, piece), F32)
        for p in range(S):
            b, o = (p * ks) // kt, (p * ks) % kt
            left = nbuf[b, at, o:o + ks]
            gate = gate + lax.dot_general(left, wgr[p], NT, preferred_element_type=F32)
            up = up + lax.dot_general(left, wur[p], NT, preferred_element_type=F32)
        return (gate / (1.0 + jnp.exp(-gate)) * up).astype(BF16)

    def stage_core(d, hidden):
        at = at_z(d)
        for p in range(S):
            b, o = (p * ks) // kt, (p * ks) % kt
            pbuf[b, at, o:o + ks] = jnp.dot(
                hidden, wdr[p], preferred_element_type=F32
            ).astype(BF16)
        first[d] = []
        for e in range(1, C):
            for w in range(Y):
                theirs = w * C + lax.rem(c + e, C)
                first[d].append(
                    (w, e, send(pbuf.at[theirs, at], rc.at[d, e - 1, w], tp=y * C + lax.rem(c + e, C)))
                )

    def stage_y(d):
        at = at_z(d)
        for _, _, copy in first[d]:
            copy.wait_recv()
        for w in range(Y):
            acc = pbuf[w * C + c, at, :].astype(F32)
            for e in range(1, C):
                acc = acc + rc[d, e - 1, w].astype(F32)
            pbuf[w * C + c, at, :] = acc.astype(BF16)
        second[d] = []
        for e in range(1, Y):
            to = lax.rem(y + e, Y) * C + c
            second[d].append(send(pbuf.at[to, at], ry.at[d, e - 1], tp=to))

    def stage_x(d):
        at = at_z(d)
        acc = pbuf[t, at, :].astype(F32)
        for e in range(1, Y):
            second[d][e - 1].wait_recv()
            acc = acc + ry[d, e - 1].astype(F32)
        pbuf[t, at, :] = acc.astype(BF16)
        third[d] = []
        for e in range(1, X):
            to = lax.rem(x + e, X)
            third[d].append(
                send(pbuf.at[t, tokens(lax.rem(z + d, Z), to)], rx.at[d, e - 1], sp=z * X + to)
            )

    def stage_z(d):
        block_at = tokens(lax.rem(z + d, Z), x)
        acc = pbuf[t, block_at, :].astype(F32)
        for e in range(1, X):
            third[d][e - 1].wait_recv()
            acc = acc + rx[d, e - 1].astype(F32)
        if d == 0:
            return acc
        pbuf[t, block_at, :] = acc.astype(BF16)
        fourth[d] = send(pbuf.at[t, block_at], rz.at[d], sp=lax.rem(z + d, Z) * X + x)

    for i, d in enumerate(order):
        hidden = stage_hidden(d)
        if i == 0:
            for copy in down_copies:
                copy.wait_recv()
        stage_core(d, hidden)
        if i:
            stage_y(order[i - 1])
    stage_y(order[-1])
    acc = None
    for i, d in enumerate(order):
        stage_x(d)
        if i:
            stage_z(order[i - 1])
    acc = stage_z(0)
    for d in range(1, Z):
        fourth[d].wait_recv()
        acc = acc + rz[d].astype(F32)
    out[...] = (mid[...].astype(F32) + 0.5 * acc).astype(BF16)
    for copy in copies:
        copy.wait_send()


def n_copies(S, T, X, C):
    Z, Y = S // X, T // C
    gather = (Z - 1) + Z * (X - 1) + S * (Y - 1) + S * (C - 1) + S * (Y - 1) * (C - 1)
    reduce = Z * (C - 1) * Y + Z * (Y - 1) + Z * (X - 1) + (Z - 1)
    return 4 * (S - 1) + 2 * (T - 1) + gather + reduce


def fused(
    S, T, signal, step_log, forget_log, damping, freq, in_re, in_im, out_re, out_im, skip, w_out,
    residual, norm_gain, w_gate, w_up, w_down,
):
    X = C = 2
    Z, Y = S // X, T // C
    rows, chans = signal.shape
    groups, states = damping.shape
    flat = groups * states
    hidden, ks = w_down.shape
    piece = hidden // S
    kt = residual.shape[1]
    twice = 128 // states

    def pair(a):
        return jnp.concatenate([a.reshape(chans, states)] * twice, axis=1)

    args = (
        signal, step_log, forget_log, damping.reshape(1, flat), freq.reshape(1, flat),
        pair(in_re.transpose(0, 2, 1)), pair(in_im.transpose(0, 2, 1)), pair(out_re), pair(out_im),
        skip.reshape(1, chans), w_out, residual, norm_gain.reshape(1, kt),
        w_gate.T, w_up.T, w_down,
    )
    n = n_copies(S, T, X, C)
    big = pltpu.VMEM((rows, flat), F32)
    landing = pltpu.VMEM((S, piece, ks), BF16)
    everything = pltpu.VMEM((T, S * rows, kt), BF16)
    vmem = pl.BlockSpec(memory_space=pltpu.VMEM)
    return pl.pallas_call(
        functools.partial(fused_kernel, S, T, X, C),
        out_shape=jax.ShapeDtypeStruct((rows, kt), BF16),
        in_specs=[vmem] * len(args),
        out_specs=vmem,
        scratch_shapes=[big] * 8 + [
            pltpu.VMEM((4, flat // 128, 128), F32),
            pltpu.VMEM((S, 4, flat // 128, 128), F32),
            pltpu.VMEM((T, rows, kt), BF16),
            pltpu.VMEM((T, rows, kt), BF16),
            pltpu.VMEM((8, rows), F32),
            pltpu.VMEM((T, 8, rows), F32),
            landing, landing, landing,
            everything,
            pltpu.VMEM((rows, kt), BF16),
            everything,
            pltpu.VMEM((Z, C - 1, Y, X * rows, kt), BF16),
            pltpu.VMEM((Z, Y - 1, X * rows, kt), BF16),
            pltpu.VMEM((Z, X - 1, rows, kt), BF16),
            pltpu.VMEM((Z, rows, kt), BF16),
            pltpu.SemaphoreType.DMA((n,)),
            pltpu.SemaphoreType.DMA((n,)),
        ],
        compiler_params=pltpu.CompilerParams(
            collective_id=0, has_side_effects=True, vmem_limit_bytes=56 * 1024 * 1024
        ),
    )(*args)


def fits(S, T, signal, damping, residual, w_down):
    states = damping.shape[1]
    width = signal.shape[1] // damping.shape[0]
    hidden, ks = w_down.shape
    rows, kt = residual.shape
    powers = all(n & (n - 1) == 0 for n in (states, width))
    return (
        S % 2 == 0 and T % 2 == 0 and S * rows * T * kt <= 4 * 1024 * 1024
        and hidden % S == 0 and (hidden // S) % 16 == 0 and ks % 128 == 0 and kt % ks == 0
        and rows % 128 == 0 and powers and states <= 128
        and (damping.size % 1024) == 0
    )


def choose(S, T, *args):
    if fits(S, T, args[0], args[3], args[11], args[15]):
        return fused(S, T, *args)
    return local(*args)


def solution(mesh):
    placed = (
        P("sp", "tp"),
        P("sp", "tp"),
        P("sp", "tp"),
        P("tp", None),
        P("tp", None),
        P("tp", None, None),
        P("tp", None, None),
        P("tp", None, None),
        P("tp", None, None),
        P("tp"),
        P("tp", None),
        P("sp", "tp"),
        P("tp"),
        P("sp", "tp"),
        P("sp", "tp"),
        P("tp", "sp"),
    )
    return jax.shard_map(
        functools.partial(choose, mesh.shape["sp"], mesh.shape["tp"]), mesh=mesh, in_specs=placed, out_specs=P("sp", "tp"), check_vma=False
    )
```

```python
import functools

import jax
import jax.numpy as jnp
from jax import lax
from jax.experimental import pallas as pl
from jax.experimental.pallas import tpu as pltpu
from jax.sharding import PartitionSpec as P

EPS = 1e-06


def entering(value, axis, join, neutral):
    count, mine = (lax.axis_size(axis), lax.axis_index(axis))
    pieces = jax.tree.map(lambda part: lax.all_gather(part, axis), value)
    subtotal = jax.tree.map(
        lambda part, zero: jnp.full_like(part, 0) + jnp.asarray(zero, part.dtype), value, neutral
    )

    def turn(position, subtotal):
        longer = join(subtotal, jax.tree.map(lambda part: part[position], pieces))
        return jax.tree.map(lambda new, old: jnp.where(position < mine, new, old), longer, subtotal)

    return lax.fori_loop(0, count - 1, turn, subtotal)


def combine(earlier, later):
    first_are, first_aim, first_bre, first_bim = earlier
    second_are, second_aim, second_bre, second_bim = later
    return (
        second_are * first_are - second_aim * first_aim,
        second_are * first_aim + second_aim * first_are,
        second_are * first_bre - second_aim * first_bim + second_bre,
        second_are * first_bim + second_aim * first_bre + second_bim,
    )


def collect(w_gate, w_up, w_down):
    gate_values_wide, up_full = (
        lax.all_gather(w_gate, "sp", axis=0, tiled=True),
        lax.all_gather(w_up, "sp", axis=0, tiled=True),
    )
    down_full = lax.all_gather(w_down, "sp", axis=1, tiled=True)
    return (gate_values_wide, up_full, down_full)


def local_states(elements, length, flat):
    span = 8
    blocks = tuple((item.reshape(length // span, span, flat) for item in elements))

    def advance(carry, block):
        collected = []
        for offset in range(span):
            carry = combine(carry, tuple((member[offset] for member in block)))
            collected.append(carry)
        stacked = tuple((jnp.stack([entry[number] for entry in collected]) for number in range(4)))
        return (carry, stacked)

    unity = jnp.ones((flat,), jnp.float32)
    nothing = jnp.zeros((flat,), jnp.float32)
    finals, stacked = lax.scan(advance, (unity, nothing, nothing, nothing), blocks)
    return (finals, tuple((member.reshape(length, flat) for member in stacked)))


def state_mixer(signal, step_log, forget_log, damping, freq, in_re, in_im, out_re, out_im, skip):
    length = signal.shape[0]
    groups, states = damping.shape
    width = in_re.shape[2]
    step = jnp.exp(step_log)[:, :, None]
    magnitude = jnp.exp(-damping[None] * step)
    angle = freq[None] * step
    decay_re = magnitude * jnp.cos(angle)
    decay_im = magnitude * jnp.sin(angle)
    denom = damping * damping + freq * freq
    factor_re = (-(decay_re - 1.0) * damping + decay_im * freq) / denom
    factor_im = (-decay_im * damping - (decay_re - 1.0) * freq) / denom
    keep = jnp.exp(forget_log)[:, :, None]
    rows = signal.reshape(length, groups, width)
    both_in = jnp.concatenate([in_re, in_im], axis=1)
    driven = jnp.einsum("tgc,gpc->tgp", rows, both_in, preferred_element_type=jnp.float32)
    source_re = driven[:, :, :states]
    source_im = driven[:, :, states:]
    drive_re = factor_re * source_re - factor_im * source_im
    drive_im = factor_re * source_im + factor_im * source_re
    flat = groups * states
    elements = (
        (keep * decay_re).reshape(length, flat),
        (keep * decay_im).reshape(length, flat),
        drive_re.reshape(length, flat),
        drive_im.reshape(length, flat),
    )
    finals, (running_real, cum_im, local_re, local_im) = local_states(elements, length, flat)
    unity = jnp.ones((flat,), jnp.float32)
    nothing = jnp.zeros((flat,), jnp.float32)
    prior = entering(finals, "sp", combine, (unity, nothing, nothing, nothing))
    state_re = local_re + running_real * prior[2][None] - cum_im * prior[3][None]
    state_im = local_im + running_real * prior[3][None] + cum_im * prior[2][None]
    state_readout = jnp.einsum(
        "myq,yzq->myz",
        state_re.reshape(length, groups, states),
        out_re.astype(jnp.float32),
        precision=lax.Precision.HIGHEST,
    ) - jnp.einsum(
        "myq,yzq->myz",
        state_im.reshape(length, groups, states),
        out_im.astype(jnp.float32),
        precision=lax.Precision.HIGHEST,
    )
    value = state_readout.reshape(length, groups * width) + skip * signal.astype(jnp.float32)
    return jax.nn.gelu(value).astype(jnp.bfloat16)


def local(
    signal,
    step_log,
    forget_log,
    damping,
    freq,
    in_re,
    in_im,
    out_re,
    out_im,
    skip,
    w_out,
    residual,
    norm_gain,
    w_gate,
    w_up,
    w_down,
):
    mixed = state_mixer(
        signal, step_log, forget_log, damping, freq, in_re, in_im, out_re, out_im, skip
    )
    partial_value = jnp.dot(mixed, w_out, preferred_element_type=jnp.float32)
    gate_values_wide, up_full, down_full = collect(w_gate, w_up, w_down)
    model_width = w_out.shape[1]
    projected = lax.psum_scatter(
        partial_value.astype(jnp.bfloat16), "tp", scatter_dimension=1, tiled=True
    ).astype(jnp.float32)
    middle = (residual.astype(jnp.float32) + projected).astype(jnp.bfloat16)
    middle_wide = middle.astype(jnp.float32)
    squares = lax.psum(jnp.sum(middle_wide * middle_wide, axis=1), "tp")
    normed = (
        middle_wide
        * lax.rsqrt(squares[:, None] / model_width + EPS)
        * norm_gain.astype(jnp.float32)
    ).astype(jnp.bfloat16)
    piece = lax.all_gather(normed, "tp", axis=1, tiled=True)
    gate = jnp.dot(piece, gate_values_wide, preferred_element_type=jnp.float32)
    up_projected = jnp.dot(piece, up_full, preferred_element_type=jnp.float32)
    hidden = (jax.nn.silu(gate) * up_projected).astype(jnp.bfloat16)
    down_terms = jnp.dot(hidden, down_full, preferred_element_type=jnp.float32)
    down = lax.psum_scatter(
        down_terms.astype(jnp.bfloat16), "tp", scatter_dimension=1, tiled=True
    ).astype(jnp.float32)
    return (middle_wide + 0.5 * down).astype(jnp.bfloat16)

MESH = pl.DeviceIdType.MESH
PUMP = (7, 7, 0, 0, 7, 0)
F32 = jnp.float32
BF16 = jnp.bfloat16
NT = (((1,), (1,)), ((), ()))


def sincos(angle):
    turns = jnp.floor(angle * 0.6366197723675814 + 0.5)
    r = angle - turns * 1.5703125
    r = r - turns * 4.837512969970703125e-4
    r = r - turns * 7.54978995489188216e-8
    q = turns.astype(jnp.int32)
    r2 = r * r
    s = ((-1.9515295891e-4 * r2 + 8.3321608736e-3) * r2 - 1.6666654611e-1) * r2 * r + r
    c = (
        ((2.443315711809948e-5 * r2 - 1.388731625493765e-3) * r2 + 4.166664568298827e-2) * r2 * r2
        - 0.5 * r2
        + 1.0
    )
    swap = (q & 1) == 1
    sine = jnp.where(swap, c, s)
    cosine = jnp.where(swap, s, c)
    sine = jnp.where((q & 2) == 2, -sine, sine)
    cosine = jnp.where(((q + 1) & 2) == 2, -cosine, cosine)
    return sine, cosine


def log2(n):
    return n.bit_length() - 1


def fused_kernel(
    S, T, X, C,
    signal, step_log, forget_log, damping, freq, b_re, b_im, c_re, c_im, skip, w_out, residual, gain,
    wg, wu, wd, out,
    stepx, keepx, dre, dim, lre, lim, rre, rim, fin, finr, part, partr, ssq, ssqr,
    wgr, wur, wdr, nbuf, mid, pbuf, rc, ry, rx, rz, send_sems, recv_sems,
):
    Z, Y = S // X, T // C
    s, t = lax.axis_index("sp"), lax.axis_index("tp")
    z, x = lax.div(s, X), lax.rem(s, X)
    y, c = lax.div(t, C), lax.rem(t, C)
    rows, chans = signal.shape
    groups, states = damping.shape
    flat, width = groups * states, chans // groups
    piece, ks = wgr.shape[1:]
    kt = nbuf.shape[2]
    model = T * kt
    count = [0]
    copies = []

    def send(src, dst, **where):
        k = count[0]
        count[0] += 1
        copy = pltpu.make_async_remote_copy(
            src_ref=src, dst_ref=dst, send_sem=send_sems.at[k], recv_sem=recv_sems.at[k],
            device_id=where, device_id_type=MESH,
        )
        copy.start()
        copies.append(copy)
        return copy

    barrier = pltpu.get_barrier_semaphore()
    for d in range(1, S):
        pl.semaphore_signal(barrier, inc=1, device_id={"sp": lax.rem(s + d, S)}, device_id_type=MESH)
    for d in range(1, T):
        pl.semaphore_signal(barrier, inc=1, device_id={"tp": lax.rem(t + d, T)}, device_id_type=MESH)
    pl.semaphore_wait(barrier, S + T - 2)

    pending = [(w, r, d) for w, r in ((wg, wgr), (wu, wur), (wd, wdr)) for d in range(1, S)]
    weight_copies = []

    def pump(number):
        for _ in range(min(number, len(pending))):
            w, r, d = pending.pop(0)
            to = lax.rem(s + d, S)
            weight_copies.append(send(w.at[pl.ds(to * piece, piece)], r.at[s], sp=to))

    pump(PUMP[0])
    for w, r in ((wg, wgr), (wu, wur), (wd, wdr)):
        r[s] = w[pl.ds(pl.multiple_of(s * piece, 16), piece)]

    lane = lax.broadcasted_iota(jnp.int32, (groups, flat), 1)
    grow = lax.broadcasted_iota(jnp.int32, (groups, flat), 0)
    onehot = jnp.where((lane >> log2(states)) == grow, 1.0, 0.0).astype(F32)
    mine_only = (lane >> log2(states)) == grow

    def flatten(ref):
        tiled = jnp.concatenate([ref[...]] * groups, axis=1)
        return jnp.sum(jnp.where(mine_only, tiled, 0.0), axis=0, keepdims=True)

    damp, rate = flatten(damping), flatten(freq)
    for log_ref, wide_ref in ((step_log, stepx), (forget_log, keepx)):
        wide_ref[...] = lax.dot_general(
            jnp.exp(log_ref[...]), onehot, (((0,), (0,)), ((), ())),
            precision=lax.Precision.HIGHEST, preferred_element_type=F32,
        )
    wide = lax.broadcasted_iota(jnp.int32, (chans, flat), 1) >> log2(states)
    tall = lax.broadcasted_iota(jnp.int32, (chans, flat), 0) >> log2(width)
    own = wide == tall

    def block_diagonal(ref):
        value = ref[...].astype(F32)
        value = jnp.concatenate([value] * (flat // value.shape[1]), axis=1)
        return jnp.where(own, value, 0.0).astype(BF16)

    dre[...] = jnp.dot(signal[...], block_diagonal(b_re), preferred_element_type=F32)
    dim[...] = jnp.dot(signal[...], block_diagonal(b_im), preferred_element_type=F32)
    denom = damp * damp + rate * rate
    dn, fn = damp / denom, rate / denom
    sub = lax.broadcasted_iota(jnp.int32, (8, flat), 0)

    def block(i, carry):
        at = pl.ds(pl.multiple_of(i * 8, 8), 8)
        st, kp = stepx[at, :], keepx[at, :]
        mag = jnp.exp(-damp * st)
        sine, cosine = sincos(rate * st)
        zr, zi = mag * cosine, mag * sine
        fr = zi * fn - (zr - 1.0) * dn
        fi = -zi * dn - (zr - 1.0) * fn
        sr, si = dre[at, :], dim[at, :]
        value = (kp * zr, kp * zi, fr * sr - fi * si, fr * si + fi * sr)
        for d in (1, 2, 4):
            ok = sub >= d
            before = tuple(
                jnp.where(ok, pltpu.roll(v, d, 0), n) for v, n in zip(value, (1.0, 0.0, 0.0, 0.0))
            )
            value = combine(before, value)
        value = combine(carry, value)
        rre[at, :], rim[at, :], lre[at, :], lim[at, :] = value
        return tuple(v[7:8, :] for v in value)

    one, nil = jnp.ones((1, flat), F32), jnp.zeros((1, flat), F32)
    final = lax.fori_loop(0, rows // 8, block, (one, nil, nil, nil))
    fold = flat // 128
    for a in range(4):
        for k in range(fold):
            fin[a, k:k + 1, :] = final[a][:, k * 128:(k + 1) * 128]
    final_copies = []
    for d in range(1, S):
        final_copies.append(send(fin, finr.at[s], sp=lax.rem(s + d, S)))
    pump(PUMP[1])
    for copy in final_copies:
        copy.wait_recv()
    prior = (jnp.ones((fold, 128), F32),) + (jnp.zeros((fold, 128), F32),) * 3
    for p in range(S - 1):
        longer = combine(prior, tuple(finr[p, a] for a in range(4)))
        prior = tuple(jnp.where(p < s, n, o) for n, o in zip(longer, prior))
    pre, pim = (
        jnp.concatenate([v[k:k + 1, :] for k in range(fold)], axis=1) for v in prior[2:]
    )

    @pl.loop(0, rows // 32)
    def _(i):
        at = pl.ds(pl.multiple_of(i * 32, 32), 32)
        ar, ai = rre[at, :], rim[at, :]
        lre[at, :] = lre[at, :] + ar * pre - ai * pim
        lim[at, :] = lim[at, :] + ar * pim + ai * pre

    def readout(state, matrix):
        high = state.astype(BF16)
        low = (state - high.astype(F32)).astype(BF16)
        return lax.dot_general(high, matrix, NT, preferred_element_type=F32) + lax.dot_general(
            low, matrix, NT, preferred_element_type=F32
        )

    value = readout(lre[...], block_diagonal(c_re)) - readout(lim[...], block_diagonal(c_im))
    value = value + skip[...] * signal[...].astype(F32)
    mixed = jax.nn.gelu(value).astype(BF16)

    part_copies = []
    for b in range(T):
        part[b] = jnp.dot(
            mixed, w_out[:, b * kt:(b + 1) * kt], preferred_element_type=F32
        ).astype(BF16)
    for d in range(1, T):
        to = lax.rem(t + d, T)
        part_copies.append(send(part.at[to], partr.at[d], tp=to))
    pump(PUMP[2])
    total = part[t].astype(F32)
    for d in range(1, T):
        part_copies[d - 1].wait_recv()
        total = total + partr[d].astype(F32)
    middle = (residual[...].astype(F32) + total).astype(BF16)
    mid[...] = middle
    wide_mid = middle.astype(F32)
    ssq[...] = lax.dot_general(
        jnp.ones((8, kt), F32), wide_mid * wide_mid, NT,
        precision=lax.Precision.HIGHEST, preferred_element_type=F32,
    )
    ssq_copies = [send(ssq, ssqr.at[d], tp=lax.rem(t + d, T)) for d in range(1, T)]
    pump(PUMP[3])
    squares = ssq[...]
    for d in range(1, T):
        ssq_copies[d - 1].wait_recv()
        squares = squares + ssqr[d]
    eye = lax.broadcasted_iota(jnp.int32, (rows, rows), 0) == lax.broadcasted_iota(
        jnp.int32, (rows, rows), 1
    )
    squares = jnp.sum(jnp.where(eye, squares[0:1, :], 0.0), axis=1, keepdims=True)
    normed = mid[...].astype(F32) * lax.rsqrt(squares / model + EPS) * gain[...].astype(F32)
    here = pl.ds(pl.multiple_of(s * rows, rows), rows)
    nbuf[t, here, :] = normed.astype(BF16)

    def tokens(zz, xx):
        return pl.ds(pl.multiple_of((zz * X + xx) * rows, rows), rows)

    def pass_on(block_ref, **where):
        return send(block_ref, block_ref, **where)

    mine = nbuf.at[t, here]
    z_copies = [None] + [
        pass_on(mine, sp=lax.rem(z + d, Z) * X + x) for d in range(1, Z)
    ]
    pump(PUMP[4])
    across = [(e, z * X + lax.rem(x + e, X)) for e in range(1, X)]
    ups = [(e, lax.rem(y + e, Y) * C + c) for e in range(1, Y)]
    mates = [(e, y * C + lax.rem(c + e, C)) for e in range(1, C)]
    y_copies, c_copies = [], {d: [] for d in range(Z)}

    def to_tp(chunk, zz, xx):
        block_ref = nbuf.at[t, tokens(zz, xx)]
        for e, to in ups:
            back = lax.rem(y - e + Y, Y) * C + c
            y_copies.append((chunk, pass_on(block_ref, tp=to), nbuf.at[back, tokens(zz, xx)]))
        for e, to in mates:
            c_copies[chunk].append(pass_on(block_ref, tp=to))

    done = [0]
    span = X * rows
    hiddens = {}

    def at_z(d):
        return pl.ds(pl.multiple_of(lax.rem(z + d, Z) * span, span), span)

    def stage_hidden(d):
        at = at_z(d)
        gate = jnp.zeros((span, piece), F32)
        up = jnp.zeros((span, piece), F32)
        for p in range(S):
            b, o = (p * ks) // kt, (p * ks) % kt
            left = nbuf[b, at, o:o + ks]
            gate = gate + lax.dot_general(left, wgr[p], NT, preferred_element_type=F32)
            up = up + lax.dot_general(left, wur[p], NT, preferred_element_type=F32)
        return (gate / (1.0 + jnp.exp(-gate)) * up).astype(BF16)

    def compute(chunk):
        for copy in c_copies[chunk]:
            copy.wait_recv()
        if chunk == 0:
            for copy in weight_copies[:2 * (S - 1)]:
                copy.wait_recv()
        hiddens[chunk] = stage_hidden((Z - chunk) % Z)


    def flush_y(upto):
        while done[0] < upto:
            chunk, copy, block_ref = y_copies[done[0]]
            copy.wait_recv()
            for e, to in mates:
                c_copies[chunk].append(pass_on(block_ref, tp=to))
            done[0] += 1

    for d in range(Z):
        zz = lax.rem(z - d + Z, Z)
        if d:
            z_copies[d].wait_recv()
        x_copies = [
            pass_on(nbuf.at[t, tokens(zz, x)], sp=z * X + lax.rem(x + e, X)) for e in range(1, X)
        ]
        to_tp(d, zz, x)
        for e in range(1, X):
            x_copies[e - 1].wait_recv()
            to_tp(d, zz, lax.rem(x - e + X, X))
        flush_y(len(y_copies) - X * (Y - 1))
        pump(PUMP[5] if d < Z - 1 else len(pending))
        if d:
            compute(d - 1)
    flush_y(len(y_copies))
    compute(Z - 1)

    order = [(Z - d) % Z for d in range(Z)]
    first, second, third, fourth = {}, {}, {}, {}

    def stage_core(d, hidden):
        at = at_z(d)
        for p in range(S):
            b, o = (p * ks) // kt, (p * ks) % kt
            pbuf[b, at, o:o + ks] = jnp.dot(
                hidden, wdr[p], preferred_element_type=F32
            ).astype(BF16)
        first[d] = []
        for e in range(1, C):
            for w in range(Y):
                theirs = w * C + lax.rem(c + e, C)
                first[d].append(
                    (w, e, send(pbuf.at[theirs, at], rc.at[d, e - 1, w], tp=y * C + lax.rem(c + e, C)))
                )

    def stage_y(d):
        at = at_z(d)
        for _, _, copy in first[d]:
            copy.wait_recv()
        for w in range(Y):
            acc = pbuf[w * C + c, at, :].astype(F32)
            for e in range(1, C):
                acc = acc + rc[d, e - 1, w].astype(F32)
            pbuf[w * C + c, at, :] = acc.astype(BF16)
        second[d] = []
        for e in range(1, Y):
            to = lax.rem(y + e, Y) * C + c
            second[d].append(send(pbuf.at[to, at], ry.at[d, e - 1], tp=to))

    def stage_x(d):
        at = at_z(d)
        acc = pbuf[t, at, :].astype(F32)
        for e in range(1, Y):
            second[d][e - 1].wait_recv()
            acc = acc + ry[d, e - 1].astype(F32)
        pbuf[t, at, :] = acc.astype(BF16)
        third[d] = []
        for e in range(1, X):
            to = lax.rem(x + e, X)
            third[d].append(
                send(pbuf.at[t, tokens(lax.rem(z + d, Z), to)], rx.at[d, e - 1], sp=z * X + to)
            )

    def stage_z(d):
        block_at = tokens(lax.rem(z + d, Z), x)
        acc = pbuf[t, block_at, :].astype(F32)
        for e in range(1, X):
            third[d][e - 1].wait_recv()
            acc = acc + rx[d, e - 1].astype(F32)
        if d == 0:
            return acc
        pbuf[t, block_at, :] = acc.astype(BF16)
        fourth[d] = send(pbuf.at[t, block_at], rz.at[d], sp=lax.rem(z + d, Z) * X + x)

    for i, d in enumerate(order):
        hidden = hiddens[i]
        if i == 0:
            for copy in weight_copies[2 * (S - 1):]:
                copy.wait_recv()
        stage_core(d, hidden)
        if i:
            stage_y(order[i - 1])
    stage_y(order[-1])
    acc = None
    for i, d in enumerate(order):
        stage_x(d)
        if i > 1:
            stage_z(order[i - 1])
    stage_z(order[-1])
    acc = stage_z(0)
    for d in range(1, Z):
        fourth[d].wait_recv()
        acc = acc + rz[d].astype(F32)
    out[...] = (mid[...].astype(F32) + 0.5 * acc).astype(BF16)
    for copy in copies:
        copy.wait_send()


def n_copies(S, T, X, C):
    Z, Y = S // X, T // C
    gather = (Z - 1) + Z * (X - 1) + S * (Y - 1) + S * (C - 1) + S * (Y - 1) * (C - 1)
    reduce = Z * (C - 1) * Y + Z * (Y - 1) + Z * (X - 1) + (Z - 1)
    return 4 * (S - 1) + 2 * (T - 1) + gather + reduce


def fused(
    S, T, signal, step_log, forget_log, damping, freq, in_re, in_im, out_re, out_im, skip, w_out,
    residual, norm_gain, w_gate, w_up, w_down,
):
    X = C = 2
    Z, Y = S // X, T // C
    rows, chans = signal.shape
    groups, states = damping.shape
    flat = groups * states
    hidden, ks = w_down.shape
    piece = hidden // S
    kt = residual.shape[1]
    twice = 128 // states

    def pair(a):
        return jnp.concatenate([a.reshape(chans, states)] * twice, axis=1)

    args = (
        signal, step_log.T, forget_log.T, damping, freq,
        pair(in_re.transpose(0, 2, 1)), pair(in_im.transpose(0, 2, 1)), pair(out_re), pair(out_im),
        skip.reshape(1, chans), w_out, residual, norm_gain.reshape(1, kt),
        w_gate.T, w_up.T, w_down,
    )
    n = n_copies(S, T, X, C)
    big = pltpu.VMEM((rows, flat), F32)
    landing = pltpu.VMEM((S, piece, ks), BF16)
    everything = pltpu.VMEM((T, S * rows, kt), BF16)
    vmem = pl.BlockSpec(memory_space=pltpu.VMEM)
    return pl.pallas_call(
        functools.partial(fused_kernel, S, T, X, C),
        out_shape=jax.ShapeDtypeStruct((rows, kt), BF16),
        in_specs=[vmem] * len(args),
        out_specs=vmem,
        scratch_shapes=[big] * 8 + [
            pltpu.VMEM((4, flat // 128, 128), F32),
            pltpu.VMEM((S, 4, flat // 128, 128), F32),
            pltpu.VMEM((T, rows, kt), BF16),
            pltpu.VMEM((T, rows, kt), BF16),
            pltpu.VMEM((8, rows), F32),
            pltpu.VMEM((T, 8, rows), F32),
            landing, landing, landing,
            everything,
            pltpu.VMEM((rows, kt), BF16),
            everything,
            pltpu.VMEM((Z, C - 1, Y, X * rows, kt), BF16),
            pltpu.VMEM((Z, Y - 1, X * rows, kt), BF16),
            pltpu.VMEM((Z, X - 1, rows, kt), BF16),
            pltpu.VMEM((Z, rows, kt), BF16),
            pltpu.SemaphoreType.DMA((n,)),
            pltpu.SemaphoreType.DMA((n,)),
        ],
        compiler_params=pltpu.CompilerParams(
            collective_id=0, has_side_effects=True, vmem_limit_bytes=56 * 1024 * 1024
        ),
    )(*args)


def fits(S, T, signal, damping, residual, w_down):
    states = damping.shape[1]
    width = signal.shape[1] // damping.shape[0]
    hidden, ks = w_down.shape
    rows, kt = residual.shape
    powers = all(n & (n - 1) == 0 for n in (states, width))
    return (
        S % 2 == 0 and T % 2 == 0 and S * rows * T * kt <= 4 * 1024 * 1024
        and hidden % S == 0 and (hidden // S) % 16 == 0 and ks % 128 == 0 and kt % ks == 0
        and rows % 128 == 0 and powers and states <= 128
        and (damping.size % 1024) == 0
    )


def choose(S, T, *args):
    if fits(S, T, args[0], args[3], args[11], args[15]):
        return fused(S, T, *args)
    return local(*args)


def solution(mesh):
    placed = (
        P("sp", "tp"),
        P("sp", "tp"),
        P("sp", "tp"),
        P("tp", None),
        P("tp", None),
        P("tp", None, None),
        P("tp", None, None),
        P("tp", None, None),
        P("tp", None, None),
        P("tp"),
        P("tp", None),
        P("sp", "tp"),
        P("tp"),
        P("sp", "tp"),
        P("sp", "tp"),
        P("tp", "sp"),
    )
    return jax.shard_map(
        functools.partial(choose, mesh.shape["sp"], mesh.shape["tp"]), mesh=mesh, in_specs=placed, out_specs=P("sp", "tp"), check_vma=False
    )
```
